1024 devices in a mesh: ep: 64 (over z, core), tp: 16 (over y, x).
Axes of the slice: x: 4, y: 4, z: 32, core: 2. Of those that a mesh axis runs over, the one named last changes fastest.
Arguments:
- tokens: bfloat16 [32768, 2048], P('ep', 'tp'), may hold values from -3000 to 3000
- norm_gain: float32 [2048], replicated, may hold values from 0.1 to 1.9
- gate_weight: bfloat16 [64, 2048, 512], P('ep'), may hold values from -0.125 to 0.125
- up_weight: bfloat16 [64, 2048, 512], P('ep'), may hold values from -0.125 to 0.125
- down_weight: bfloat16 [64, 512, 2048], P('ep'), may hold values from -0.25 to 0.25
- expert_ids: int32 [32768, 2], P('ep'), may hold values from 0 to 63, as said below
- route_weight: float32 [32768, 2], P('ep'), may hold values from 0.2 to 1
Outputs:
- mixed: bfloat16 [32768, 2048], P('ep', 'tp')
The draws below stay inside these ranges and needn't reach their ends.
Inputs may be any that keep to these rules, and one draw needn't show every extreme that they name: `expert_ids`: A token's two experts differ and lie in one group of 8 consecutive experts. In each aligned block of 32 rows no expert is named more than 2 times, and in every block all experts of one group, the same group for all blocks, are named exactly 2 times.
All inputs are finite; a program needn't handle non-finite values.
Results may differ from the reference program's by a relative error of at most 0.0071.
Values may be sent and summed in bfloat16 or wider, within the bound.
A program may use at most 32 MiB of HBM per device.

```python
import math
import jax
import jax.numpy as jnp
from jax import lax

D = 2048
FF = 512
TOK_DEV = 32
EXPERTS = 64
EPG = 8
GROUPS = 8
CAP = 2
GCAP = 8
TOKENS = 32768


def group_order(order_key):
    return jax.random.permutation(order_key, EPG)


def route_block(block_key, hot_group):
    keys = jax.random.split(block_key, 5)
    group_bias = jax.random.randint(keys[0], (GROUPS,), 1, 5)
    slot_group = jnp.arange(GROUPS * GCAP, dtype=jnp.int32) // GCAP
    score = jax.random.randint(keys[1], (GROUPS * GCAP,), 0, 65536) * group_bias[slot_group]
    score = jnp.where(slot_group == hot_group, 4194304, score)
    score = score * (GROUPS * GCAP) + jnp.arange(GROUPS * GCAP, dtype=jnp.int32)
    unused, chosen = lax.top_k(score, TOK_DEV)
    chosen = chosen[jax.random.permutation(keys[2], TOK_DEV)]
    group_of = chosen // GCAP
    within = chosen % GCAP
    orders = jax.vmap(group_order)(jax.random.split(keys[3], GROUPS))
    offsets = jax.random.randint(keys[4], (GROUPS, CAP // 2), 1, EPG)
    position = within % EPG
    first = orders[group_of, position]
    second = orders[group_of, (position + offsets[group_of, within // EPG]) % EPG]
    return jnp.stack([group_of * EPG + first, group_of * EPG + second], axis=1).astype(jnp.int32)


def draw_expert_ids(key, part):
    hot_group = jax.random.randint(jax.random.fold_in(key, 11), (), 0, GROUPS)
    block_keys = jax.random.split(jax.random.fold_in(key, 12), TOKENS // TOK_DEV)
    blocks = jax.vmap(route_block, in_axes=(0, None))(block_keys, hot_group)
    return blocks.reshape(TOKENS, 2)


def draw_tokens(key, part):
    keys = jax.random.split(jax.random.fold_in(key, 21), 4)
    column_rise = jnp.exp(jnp.log(10.0) * jnp.arange(D, dtype=jnp.float32) / D)
    column_rough = jnp.exp(jax.random.uniform(keys[0], (D,), jnp.float32, -0.5, 0.5))
    row_scale = jnp.exp(jax.random.uniform(keys[1], (TOKENS, 1), jnp.float32, 0.0, jnp.log(10.0)))
    base = jnp.clip(jax.random.normal(keys[3], (TOKENS, D), jnp.float32), -6.0, 6.0)
    return (base * row_scale * column_rise * column_rough).astype(jnp.bfloat16)


def shard_levels(stream_key, extent, shards, low, largest):
    loudness = 1.0
    for dim, parts in shards:
        steps = jax.random.uniform(jax.random.fold_in(jax.random.fold_in(stream_key, 6), dim), (parts,), jnp.float32, low / len(shards), largest / len(shards))
        loudness = loudness * jnp.repeat(jnp.exp(steps), extent[dim] // parts).reshape((-1,) + (1,) * (len(extent) - 1 - dim))
    return loudness


def centred(stream_key, extent, deviation, reach, cuts=(), held_as=jnp.bfloat16):
    array = jax.random.normal(stream_key, extent, jnp.float32) * deviation
    if len(cuts) > 0:
        array = shard_levels(stream_key, extent, cuts, -0.22, 0.18) * array
    return jnp.clip(array, min=-reach, max=reach).astype(held_as)


def setup_inputs(seed: int = 0) -> dict:
    key_of = jax.random.split(jax.random.key(seed), 8)
    tokens = draw_tokens(jax.random.fold_in(key_of[7], 71), 0)
    norm_gain = jnp.clip(1.0 + 0.18 * jax.random.normal(key_of[1], (D,), jnp.float32), 0.1, 1.9)
    gate_weight = centred(key_of[2], (EXPERTS, D, FF), D ** -0.5, 0.125, ((0, 64),))
    up_weight = centred(key_of[3], (EXPERTS, D, FF), D ** -0.5, 0.125, ((0, 64),))
    down_weight = centred(key_of[4], (EXPERTS, FF, D), FF ** -0.5, 0.25, ((0, 64),))
    expert_ids = draw_expert_ids(jax.random.fold_in(key_of[7], 71), 0)
    route_weight = jnp.clip(jnp.exp(math.log(1.0) - 1.609438 * jax.random.uniform(key_of[6], (TOKENS, 2), jnp.float32) ** shard_levels(key_of[6], (TOKENS, 2), ((0, 64),), -0.2, 0.2)), 0.2, 1.0)
    return {"tokens": tokens, "norm_gain": norm_gain, "gate_weight": gate_weight, "up_weight": up_weight, "down_weight": down_weight, "expert_ids": expert_ids, "route_weight": route_weight}


def reference(tokens, norm_gain, gate_weight, up_weight, down_weight, expert_ids, route_weight):
    widened = tokens.astype(jnp.float32)
    mean_square = lax.optimization_barrier(jnp.mean(widened * widened, axis=-1, keepdims=True))
    normed = (widened * lax.rsqrt(mean_square + 1e-06) * norm_gain).astype(jnp.bfloat16)
    flat_ids = expert_ids.reshape(-1)
    flat_weight = route_weight.reshape(-1)
    longest = TOKENS // TOK_DEV * CAP

    def per_expert(summed, expert):
        matches = flat_ids == expert
        places = jnp.nonzero(matches, size=longest, fill_value=0)[0].astype(jnp.int32)
        present = jnp.arange(longest, dtype=jnp.int32) < jnp.sum(matches.astype(jnp.int32))
        token_rows = places // 2
        chosen = normed[token_rows]
        gate_part = jnp.dot(chosen, gate_weight[expert], preferred_element_type=jnp.float32)
        up_part = jnp.dot(chosen, up_weight[expert], preferred_element_type=jnp.float32)
        hidden = (jax.nn.silu(gate_part) * up_part).astype(jnp.bfloat16)
        produced = jnp.dot(hidden, down_weight[expert], preferred_element_type=jnp.float32).astype(jnp.bfloat16)
        produced = lax.optimization_barrier(produced).astype(jnp.float32)
        weight_used = jnp.where(present, flat_weight[places], 0.0)
        summed = summed.at[token_rows].add(produced * weight_used[:, None])
        return (summed, None)
    summed, unused = lax.scan(per_expert, jnp.zeros((TOKENS, D), jnp.float32), jnp.arange(EXPERTS, dtype=jnp.int32))
    return summed.astype(jnp.bfloat16)
```

```python
from functools import partial

import jax
import jax.numpy as jnp
from jax import lax
from jax.experimental import pallas as pl
from jax.experimental.pallas import tpu as pltpu
from jax.sharding import PartitionSpec as P

MESH = pl.DeviceIdType.MESH
F32 = jnp.float32
BF16 = jnp.bfloat16
CHIPS = 4
EPG = 8
SLOTS = 8


def dot(a, b, contract=((1,), (0,))):
    return lax.dot_general(a, b, (contract, ((), ())), preferred_element_type=F32)


def to_row(col):
    n = col.shape[0]
    eye = lax.broadcasted_iota(jnp.int32, (n, n), 0) == lax.broadcasted_iota(jnp.int32, (n, n), 1)
    return jnp.sum(jnp.where(eye, col, jnp.zeros_like(col)), axis=0, keepdims=True)


def body(
    ep_count, tp_count,
    tokens, gain, gate_hbm, up_hbm, down_hbm, ids_hbm, wts_hbm,
    out,
    xin, ids, wts, gate, up, down, xn, sb, rbuf, sbuf, xe, yo, pbuf, obuf, ret, mx,
    w_sem, in_sem, tp_send, tp_recv, s1, r1, s2, r2, s3, r3, s4, r4, fin_send, fin_recv,
):
    e = lax.axis_index("ep")
    t = lax.axis_index("tp")
    groups = ep_count // EPG
    half = groups // 2
    nbatch = half
    c = lax.rem(e, 2)
    z = e // 2
    p = lax.rem(z, CHIPS)
    g = z // CHIPS
    rows = xn.shape[0]
    width = gate.shape[0]
    is_relay = lax.rem(p, 3) == 0
    my_e = 2 * p + c

    weight_copies = [
        pltpu.make_async_copy(gate_hbm.at[0], gate, w_sem.at[0]),
        pltpu.make_async_copy(up_hbm.at[0], up, w_sem.at[1]),
        pltpu.make_async_copy(down_hbm.at[0], down, w_sem.at[2]),
    ]
    small_copies = [
        pltpu.make_async_copy(ids_hbm.at[pl.ds(t * rows, rows)], ids, in_sem.at[0]),
        pltpu.make_async_copy(wts_hbm.at[pl.ds(t * rows, rows)], wts, in_sem.at[1]),
        pltpu.make_async_copy(tokens.at[pl.ds(t * rows, rows)], xin.at[t], in_sem.at[2]),
    ]
    for cp in small_copies:
        cp.start()
    barrier = pltpu.get_barrier_semaphore()

    @pl.loop(1, ep_count)
    def _(k):
        pl.semaphore_signal(barrier, inc=1, device_id={"ep": lax.rem(e + k, ep_count)}, device_id_type=MESH)

    if tp_count > 1:
        @pl.loop(1, tp_count)
        def _(k):
            pl.semaphore_signal(barrier, inc=1, device_id={"tp": lax.rem(t + k, tp_count)}, device_id_type=MESH)

    for cp in weight_copies:
        cp.start()

    for cp in small_copies[:2]:
        cp.wait()
    idv = ids[...]
    wv = wts[...]
    lane2 = lax.broadcasted_iota(jnp.int32, idv.shape, 1)
    id_col = [jnp.sum(jnp.where(lane2 == k, idv, 0), axis=1, keepdims=True) for k in range(2)]
    w_col = [jnp.sum(jnp.where(lane2 == k, wv, 0.0), axis=1, keepdims=True) for k in range(2)]
    id_row = [to_row(v) for v in id_col]
    before = lax.broadcasted_iota(jnp.int32, (rows, rows), 1) < lax.broadcasted_iota(jnp.int32, (rows, rows), 0)
    g_col = id_col[0] // EPG
    same = before & ((id_row[0] // EPG) == g_col)
    rank = jnp.sum(jnp.where(same, 1, 0), axis=1, keepdims=True)
    rel = lax.rem(g_col - g + groups, groups)
    target = rel * SLOTS + rank
    q_col = []
    for k in range(2):
        hit = jnp.where(id_row[0] == id_col[k], 1, 0) + jnp.where(id_row[1] == id_col[k], 1, 0)
        q_col.append(jnp.sum(jnp.where(before, hit, 0), axis=1, keepdims=True))
    lane = lax.broadcasted_iota(jnp.int32, (rows, 128), 1)
    lane_lo = lax.rem(lane, 64)
    w_tok = jnp.zeros((rows, 128), F32)
    for k in range(2):
        high = w_col[k].astype(BF16).astype(F32)
        part = jnp.where(lane < 64, high, w_col[k] - high)
        on = (lane_lo // 8 == lax.rem(id_col[k], EPG)) & (lax.rem(lane, 2) == q_col[k])
        w_tok = w_tok + jnp.where(on, part, 0.0)
    xn[:, width:] = w_tok.astype(BF16)
    place = jnp.where(
        lax.broadcasted_iota(jnp.int32, (groups * SLOTS, rows), 0) == to_row(target), 1.0, 0.0
    ).astype(BF16)
    unplace = jnp.where(
        lax.broadcasted_iota(jnp.int32, (rows, groups * SLOTS), 1) == target, 1.0, 0.0
    ).astype(BF16)

    pl.semaphore_wait(barrier, ep_count - 1 + (tp_count - 1))

    if tp_count > 1:
        @pl.loop(1, tp_count)
        def _(k):
            peer = lax.rem(t + k, tp_count)
            pltpu.make_async_remote_copy(
                src_ref=tokens.at[pl.ds(peer * rows, rows)], dst_ref=xin.at[t],
                send_sem=tp_send, recv_sem=tp_recv, device_id={"tp": peer}, device_id_type=MESH,
            ).start()

        pltpu.make_async_copy(xin.at[pl.ds(0, tp_count - 1)], xin.at[pl.ds(0, tp_count - 1)], tp_recv).wait()
    small_copies[2].wait()
    piece = xin.shape[2]
    total = jnp.zeros((rows, piece), F32)
    for i in range(tp_count):
        v = xin[i].astype(F32)
        total = total + v * v
    scale = lax.rsqrt(jnp.sum(total, axis=1, keepdims=True) / width + 1e-06)
    for i in range(tp_count):
        cols = slice(i * piece, (i + 1) * piece)
        xn[:, cols] = (xin[i].astype(F32) * scale * gain[:, cols]).astype(BF16)
    placed = dot(place, xn[...])
    for r in range(groups):
        sb[r] = placed[r * SLOTS:(r + 1) * SLOTS].astype(BF16)

    def ep_of(zz):
        return {"ep": zz * 2 + c}

    def send1(r, dest_z, k, b):
        return pltpu.make_async_remote_copy(
            src_ref=sb.at[r], dst_ref=rbuf.at[k, b], send_sem=s1, recv_sem=r1.at[k],
            device_id=ep_of(dest_z), device_id_type=MESH,
        )

    send1(half, lax.rem(g + half, groups) * CHIPS + 3 * (1 - p // 2), nbatch - 1, lax.rem(p, 2)).start()
    for d in range(half - 1, 0, -1):
        send1(d, lax.rem(g + d, groups) * CHIPS, d - 1, p).start()
        send1(groups - d, lax.rem(g + groups - d, groups) * CHIPS + 3, d - 1, p).start()
    own_slot = 2 + lax.rem(p, 2)

    @pl.when(is_relay)
    def _():
        pltpu.make_async_copy(sb.at[0], rbuf.at[nbatch - 1, own_slot], r1.at[nbatch - 1]).start()

    @pl.when(jnp.logical_not(is_relay))
    def _():
        send1(0, g * CHIPS + 3 * (p // 2), nbatch - 1, own_slot).start()

    relay_id = (p // 3) * 2 + c
    row_of = lax.broadcasted_iota(jnp.int32, (32, 64), 0) // SLOTS
    lane_of = lax.rem(lax.broadcasted_iota(jnp.int32, (32, 64), 1) // 2, 4)
    diagonal = row_of == lane_of

    def select(k):
        pltpu.make_async_copy(rbuf.at[k], rbuf.at[k], r1.at[k]).wait()
        got = rbuf[k].reshape(4 * SLOTS, width + 128)
        wide = got[:, width:width + 64].astype(F32)
        sel = jnp.where(diagonal & (wide != 0.0), 1.0, 0.0).astype(BF16)
        chosen = dot(sel, got[:, :width], ((0,), (0,)))
        for ee in range(EPG):
            sbuf[k, ee] = chosen[ee * 8:(ee + 1) * 8].astype(BF16)
        for d in range(1, EPG):
            ee = lax.rem(my_e + d, EPG)
            pltpu.make_async_remote_copy(
                src_ref=sbuf.at[k, ee], dst_ref=xe.at[k, relay_id], send_sem=s2, recv_sem=r2.at[k],
                device_id={"ep": g * EPG + ee}, device_id_type=MESH,
            ).start()
        pltpu.make_async_copy(sbuf.at[k, my_e], xe.at[k, relay_id], r2.at[k]).start()

    def expert(k):
        pltpu.make_async_copy(xe.at[k], xe.at[k], r2.at[k]).wait()
        x = xe[k].reshape(32, width)
        a = dot(x, gate[...])
        b = dot(x, up[...])
        h = (a / (1.0 + jnp.exp(-a)) * b).astype(BF16)
        y = dot(h, down[...])
        for i in range(4):
            yo[k, i] = y[i * 8:(i + 1) * 8].astype(BF16)
        for i in range(4):
            dest = 6 * (i // 2) + i % 2

            @pl.when(my_e == dest)
            def _():
                pltpu.make_async_copy(yo.at[k, i], pbuf.at[k, my_e], r3.at[k]).start()

            @pl.when(my_e != dest)
            def _():
                pltpu.make_async_remote_copy(
                    src_ref=yo.at[k, i], dst_ref=pbuf.at[k, my_e], send_sem=s3, recv_sem=r3.at[k],
                    device_id={"ep": g * EPG + dest}, device_id_type=MESH,
                ).start()

    def combine(k):
        pltpu.make_async_copy(pbuf.at[k], pbuf.at[k], r3.at[k]).wait()
        parts = pbuf[k].reshape(64, width)
        wide = rbuf[k].reshape(4 * SLOTS, width + 128)[:, width:].astype(F32)
        high = jnp.where(diagonal, wide[:, :64], 0.0).astype(BF16)
        low = jnp.where(diagonal, wide[:, 64:], 0.0).astype(BF16)
        y = dot(high, parts) + dot(low, parts)
        for b in range(4):
            obuf[k, b] = y[b * 8:(b + 1) * 8].astype(BF16)
        sign = 1 - 2 * (p // 3)
        for b in range(4):
            if k < nbatch - 1:
                d = k + 1
                src_z = lax.rem(g + groups - sign * d, groups) * CHIPS + b
                r = lax.rem(groups + sign * d, groups)
            elif b < 2:
                src_z = lax.rem(g + half, groups) * CHIPS + 2 * (1 - p // 3) + b
                r = half
            else:
                src_z = g * CHIPS + 2 * (p // 3) + b - 2
                r = 0
            send = pltpu.make_async_remote_copy(
                src_ref=obuf.at[k, b], dst_ref=ret.at[r], send_sem=s4, recv_sem=r4,
                device_id=ep_of(src_z), device_id_type=MESH,
            )
            if k == nbatch - 1 and b >= 2:
                mine = src_z == z

                @pl.when(mine)
                def _():
                    pltpu.make_async_copy(obuf.at[k, b], ret.at[0], r4).start()

                @pl.when(jnp.logical_not(mine))
                def _():
                    send.start()
            else:
                send.start()

    for cp in weight_copies:
        cp.wait()
    order = [nbatch - 1] + list(range(nbatch - 2, -1, -1))
    for step in range(nbatch + 2):
        if step < nbatch:
            @pl.when(is_relay)
            def _():
                select(order[step])
        if 1 <= step <= nbatch:
            expert(order[step - 1])
        if step >= 2:
            @pl.when(is_relay)
            def _():
                combine(order[step - 2])

    pltpu.make_async_copy(ret, ret, r4).wait()
    mixed = dot(unplace, ret[...].reshape(groups * SLOTS, width))
    for i in range(tp_count):
        mx[i] = mixed[:, i * piece:(i + 1) * piece].astype(BF16)
    mine = pltpu.make_async_copy(mx.at[t], out.at[pl.ds(t * rows, rows)], in_sem.at[2])
    mine.start()
    if tp_count > 1:
        @pl.loop(1, tp_count)
        def _(k):
            peer = lax.rem(t + k, tp_count)
            pltpu.make_async_remote_copy(
                src_ref=mx.at[peer], dst_ref=out.at[pl.ds(t * rows, rows)],
                send_sem=fin_send, recv_sem=fin_recv, device_id={"tp": peer}, device_id_type=MESH,
            ).start()

        others = mx.at[pl.ds(0, tp_count - 1)]
        pltpu.make_async_copy(others, others, fin_recv).wait()
        pltpu.make_async_copy(others, others, fin_send).wait()
        others = xin.at[pl.ds(0, tp_count - 1)]
        pltpu.make_async_copy(others, others, tp_send).wait()
    mine.wait()

    @pl.when(is_relay)
    def _():
        n = groups - 1
        pltpu.make_async_copy(sb.at[pl.ds(0, n)], sb.at[pl.ds(0, n)], s1).wait()
        every = sbuf.at[:, pl.ds(0, EPG - 1)]
        pltpu.make_async_copy(every, every, s2).wait()
        every = yo.at[:, pl.ds(0, 3)]
        pltpu.make_async_copy(every, every, s3).wait()
        rest = nbatch * 4 - 1
        flat = obuf.reshape(nbatch * 4, SLOTS, width).at[pl.ds(0, rest)]
        pltpu.make_async_copy(flat, flat, s4).wait()

    @pl.when(jnp.logical_not(is_relay))
    def _():
        pltpu.make_async_copy(sb, sb, s1).wait()
        pltpu.make_async_copy(yo, yo, s3).wait()


def local(tokens, norm_gain, gate_weight, up_weight, down_weight, expert_ids, route_weight, ep_count, tp_count):
    tok, piece = tokens.shape
    rows = tok // tp_count
    _, width, ff = gate_weight.shape
    groups = ep_count // EPG
    nb = groups // 2
    wide = width + 128
    any_spec = pl.BlockSpec(memory_space=pl.ANY)
    vmem_spec = pl.BlockSpec(memory_space=pltpu.VMEM)
    dma = pltpu.SemaphoreType.DMA
    return pl.pallas_call(
        partial(body, ep_count, tp_count),
        out_shape=jax.ShapeDtypeStruct(tokens.shape, BF16),
        in_specs=[any_spec, vmem_spec] + [any_spec] * 5,
        out_specs=any_spec,
        scratch_shapes=[
            pltpu.VMEM((tp_count, rows, piece), BF16),
            pltpu.VMEM((rows, 2), jnp.int32),
            pltpu.VMEM((rows, 2), F32),
            pltpu.VMEM((width, ff), BF16),
            pltpu.VMEM((width, ff), BF16),
            pltpu.VMEM((ff, width), BF16),
            pltpu.VMEM((rows, wide), BF16),
            pltpu.VMEM((groups, SLOTS, wide), BF16),
            pltpu.VMEM((nb, 4, SLOTS, wide), BF16),
            pltpu.VMEM((nb, EPG, 8, width), BF16),
            pltpu.VMEM((nb, 4, 8, width), BF16),
            pltpu.VMEM((nb, 4, 8, width), BF16),
            pltpu.VMEM((nb, EPG, 8, width), BF16),
            pltpu.VMEM((nb, 4, SLOTS, width), BF16),
            pltpu.VMEM((groups, SLOTS, width), BF16),
            pltpu.VMEM((tp_count, rows, piece), BF16),
            dma((3,)), dma((3,)), dma, dma,
            dma, dma((nb,)), dma, dma((nb,)), dma, dma((nb,)), dma, dma, dma, dma,
        ],
        compiler_params=pltpu.CompilerParams(
            collective_id=0, has_side_effects=True, vmem_limit_bytes=50 * 1024 * 1024
        ),
        name="moe",
    )(tokens, norm_gain.reshape(1, width), gate_weight, up_weight, down_weight, expert_ids, route_weight)


def solution(mesh):
    in_specs = (
        P("ep", "tp"),
        P(),
        P("ep", None, None),
        P("ep", None, None),
        P("ep", None, None),
        P("ep", None),
        P("ep", None),
    )
    fn = partial(local, ep_count=mesh.shape["ep"], tp_count=mesh.shape["tp"])
    return jax.shard_map(fn, mesh=mesh, in_specs=in_specs, out_specs=P("ep", "tp"), check_vma=False)
```

```python
from functools import partial

import jax
import jax.numpy as jnp
from jax import lax
from jax.experimental import pallas as pl
from jax.experimental.pallas import tpu as pltpu
from jax.sharding import PartitionSpec as P

MESH = pl.DeviceIdType.MESH
F32 = jnp.float32
BF16 = jnp.bfloat16
CHIPS = 4
EPG = 8
SLOTS = 8
ORDER = ('D0', 'H3', 'D1', 'S0', 'S1', 'E0', 'E1', 'C1', 'C0')
NB = 2


def dot(a, b, contract=((1,), (0,))):
    return lax.dot_general(a, b, (contract, ((), ())), preferred_element_type=F32)


def to_row(col):
    n = col.shape[0]
    eye = lax.broadcasted_iota(jnp.int32, (n, n), 0) == lax.broadcasted_iota(jnp.int32, (n, n), 1)
    return jnp.sum(jnp.where(eye, col, jnp.zeros_like(col)), axis=0, keepdims=True)


def body(
    ep_count, tp_count,
    tokens, gain_hbm, gate_hbm, up_hbm, down_hbm, ids_hbm, wts_hbm,
    out,
    tok_v, xin, gain, ids, wts, gate, up, down, xn, sb, rbuf, sbuf, xe, yo, pbuf, obuf, ret, mx,
    known, w_sem, in_sem, tp_send, tp_recv, s1, r1, s2, r2, s3, r3, s4, r4, fin_send, fin_recv,
):
    e = lax.axis_index("ep")
    t = lax.axis_index("tp")
    groups = ep_count // EPG
    chips = ep_count // 2
    half = groups // 2
    c = lax.rem(e, 2)
    z = e // 2
    p = lax.rem(z, CHIPS)
    g = z // CHIPS
    rows = xn.shape[0]
    width = gate.shape[0]
    my_e = 2 * p + c

    weight_copies = [
        pltpu.make_async_copy(gate_hbm.at[0], gate, w_sem.at[0]),
        pltpu.make_async_copy(up_hbm.at[0], up, w_sem.at[1]),
        pltpu.make_async_copy(down_hbm.at[0], down, w_sem.at[2]),
    ]
    small_copies = [
        pltpu.make_async_copy(ids_hbm, ids, in_sem.at[0]),
        pltpu.make_async_copy(wts_hbm, wts, in_sem.at[1]),
        pltpu.make_async_copy(tokens, tok_v, in_sem.at[2]),
        pltpu.make_async_copy(gain_hbm, gain, in_sem.at[3]),
    ]
    for cp in small_copies:
        cp.start()
    barrier = pltpu.get_barrier_semaphore()

    def column(zz):
        return {"ep": lax.rem(zz + 2 * chips, chips) * 2 + c}

    for peer in ({"ep": z * 2 + 1 - c}, column(z + 1), column(z - 1)):
        pl.semaphore_signal(barrier, inc=1, device_id=peer, device_id_type=MESH)

    if tp_count > 1:
        @pl.loop(1, tp_count)
        def _(k):
            pl.semaphore_signal(barrier, inc=1, device_id={"tp": lax.rem(t + k, tp_count)}, device_id_type=MESH)

    for cp in weight_copies:
        cp.start()

    for cp in small_copies[:2]:
        cp.wait()
    tok = ids.shape[1]
    pick = lax.broadcasted_iota(jnp.int32, (rows, tok), 1) == (
        lax.broadcasted_iota(jnp.int32, (rows, tok), 0) + t * rows
    )
    id_col = [jnp.sum(jnp.where(pick, ids[k:k + 1, :], 0), axis=1, keepdims=True) for k in range(2)]
    w_col = [jnp.sum(jnp.where(pick, wts[k:k + 1, :], 0.0), axis=1, keepdims=True) for k in range(2)]
    id_row = [to_row(v) for v in id_col]
    before = lax.broadcasted_iota(jnp.int32, (rows, rows), 1) < lax.broadcasted_iota(jnp.int32, (rows, rows), 0)
    g_col = id_col[0] // EPG
    same = before & ((id_row[0] // EPG) == g_col)
    rank = jnp.sum(jnp.where(same, 1, 0), axis=1, keepdims=True)
    rel = lax.rem(g_col - g + groups, groups)
    target = rel * SLOTS + rank
    q_col = []
    for k in range(2):
        hit = jnp.where(id_row[0] == id_col[k], 1, 0) + jnp.where(id_row[1] == id_col[k], 1, 0)
        q_col.append(jnp.sum(jnp.where(before, hit, 0), axis=1, keepdims=True))
    lane = lax.broadcasted_iota(jnp.int32, (rows, 128), 1)
    lane_lo = lax.rem(lane, 64)
    w_tok = jnp.zeros((rows, 128), F32)
    for k in range(2):
        high = w_col[k].astype(BF16).astype(F32)
        part = jnp.where(lane < 64, high, w_col[k] - high)
        on = (lane_lo // 8 == lax.rem(id_col[k], EPG)) & (lax.rem(lane, 2) == q_col[k])
        w_tok = w_tok + jnp.where(on, part, 0.0)
    xn[:, width:] = w_tok.astype(BF16)
    place = jnp.where(
        lax.broadcasted_iota(jnp.int32, (groups * SLOTS, rows), 0) == to_row(target), 1.0, 0.0
    ).astype(BF16)
    unplace = jnp.where(
        lax.broadcasted_iota(jnp.int32, (rows, groups * SLOTS), 1) == target, 1.0, 0.0
    ).astype(BF16)

    for cp in small_copies[2:]:
        cp.wait()
    xin[t] = tok_v[pl.ds(pl.multiple_of(t * rows, rows), rows), :]
    pl.semaphore_wait(barrier, 3 + (tp_count - 1))

    if tp_count > 1:
        @pl.loop(1, tp_count)
        def _(k):
            peer = lax.rem(t + k, tp_count)
            pltpu.make_async_remote_copy(
                src_ref=tok_v.at[pl.ds(peer * rows, rows)], dst_ref=xin.at[t],
                send_sem=tp_send, recv_sem=tp_recv, device_id={"tp": peer}, device_id_type=MESH,
            ).start()

    def tell(i):
        for side in range(2):
            pl.semaphore_signal(
                known.at[2 * i + side], inc=1, device_id=column(z + (1 - 2 * side) * 2**i), device_id_type=MESH
            )

    def hear(i):
        for side in range(2):
            pl.semaphore_wait(known.at[2 * i + side], 1)

    for i in range(3):
        tell(i)
        hear(i)
    tell(3)
    if tp_count > 1:
        pltpu.make_async_copy(xin.at[pl.ds(0, tp_count - 1)], xin.at[pl.ds(0, tp_count - 1)], tp_recv).wait()
    piece = xin.shape[2]
    total = jnp.zeros((rows, piece), F32)
    for i in range(tp_count):
        v = xin[i].astype(F32)
        total = total + v * v
    scale = lax.rsqrt(jnp.sum(total, axis=1, keepdims=True) / width + 1e-06)
    for i in range(tp_count):
        cols = slice(i * piece, (i + 1) * piece)
        xn[:, cols] = (xin[i].astype(F32) * scale * gain[:, cols]).astype(BF16)
    placed = dot(place, xn[...])
    for r in range(groups):
        sb[r] = placed[r * SLOTS:(r + 1) * SLOTS].astype(BF16)

    def ep_of(zz):
        return {"ep": zz * 2 + c}

    def send1(r, dest_z, k, b):
        return pltpu.make_async_remote_copy(
            src_ref=sb.at[r], dst_ref=rbuf.at[k, b], send_sem=s1.at[k], recv_sem=r1.at[k],
            device_id=ep_of(dest_z), device_id_type=MESH,
        )

    odd = lax.rem(p, 2)

    def dispatch(k):
        if k == 1:
            send1(half, lax.rem(g + half, groups) * CHIPS + 2 * (1 - p // 2) + odd, k, 2).start()
            pltpu.make_async_copy(sb.at[0], rbuf.at[k, 3], r1.at[k]).start()
        for d in (2, 1) if k == 0 else (3,):
            b = 2 * ((d - 1) % 2) + odd
            send1(d, lax.rem(g + d, groups) * CHIPS + p // 2, k, b).start()
            send1(groups - d, lax.rem(g + groups - d, groups) * CHIPS + 2 + p // 2, k, b).start()

    def dispatched(k):
        n = 4 if k == 0 else 3
        pltpu.make_async_copy(sb.at[pl.ds(0, n)], sb.at[pl.ds(0, n)], s1.at[k]).wait()

    row_of = lax.broadcasted_iota(jnp.int32, (32, 64), 0) // SLOTS
    lane_of = lax.rem(lax.broadcasted_iota(jnp.int32, (32, 64), 1) // 2, 4)
    diagonal = row_of == lane_of

    def select(k):
        pltpu.make_async_copy(rbuf.at[k], rbuf.at[k], r1.at[k]).wait()
        got = rbuf[k].reshape(4 * SLOTS, width + 128)
        wide = got[:, width:width + 64].astype(F32)
        sel = jnp.where(diagonal & (wide != 0.0), 1.0, 0.0).astype(BF16)
        chosen = dot(sel, got[:, :width], ((0,), (0,)))
        for ee in range(EPG):
            sbuf[k, ee] = chosen[ee * 8:(ee + 1) * 8].astype(BF16)
        for d in range(1, EPG):
            ee = lax.rem(my_e + d, EPG)
            pltpu.make_async_remote_copy(
                src_ref=sbuf.at[k, ee], dst_ref=xe.at[k, my_e], send_sem=s2, recv_sem=r2.at[k],
                device_id={"ep": g * EPG + ee}, device_id_type=MESH,
            ).start()
        pltpu.make_async_copy(sbuf.at[k, my_e], xe.at[k, my_e], r2.at[k]).start()

    def expert(k):
        pltpu.make_async_copy(xe.at[k], xe.at[k], r2.at[k]).wait()
        x = xe[k].reshape(64, width)
        a = dot(x, gate[...])
        b = dot(x, up[...])
        h = (a / (1.0 + jnp.exp(-a)) * b).astype(BF16)
        y = dot(h, down[...])
        for i in range(EPG):
            yo[k, i] = y[i * 8:(i + 1) * 8].astype(BF16)
        for d in range(1, EPG):
            ee = lax.rem(my_e + d, EPG)
            pltpu.make_async_remote_copy(
                src_ref=yo.at[k, ee], dst_ref=pbuf.at[k, my_e], send_sem=s3, recv_sem=r3.at[k],
                device_id={"ep": g * EPG + ee}, device_id_type=MESH,
            ).start()
        pltpu.make_async_copy(yo.at[k, my_e], pbuf.at[k, my_e], r3.at[k]).start()

    def combine(k):
        pltpu.make_async_copy(pbuf.at[k], pbuf.at[k], r3.at[k]).wait()
        parts = pbuf[k].reshape(64, width)
        wide = rbuf[k].reshape(4 * SLOTS, width + 128)[:, width:].astype(F32)
        high = jnp.where(diagonal, wide[:, :64], 0.0).astype(BF16)
        low = jnp.where(diagonal, wide[:, 64:], 0.0).astype(BF16)
        y = dot(high, parts) + dot(low, parts)
        for b in range(4):
            obuf[k, b] = y[b * 8:(b + 1) * 8].astype(BF16)
        sign = 1 - 2 * (p // 2)

        def back(b, src_z, r):
            pltpu.make_async_remote_copy(
                src_ref=obuf.at[k, b], dst_ref=ret.at[r], send_sem=s4, recv_sem=r4,
                device_id=ep_of(src_z), device_id_type=MESH,
            ).start()

        for d in (2, 1) if k == 0 else (3,):
            for i in range(2):
                back(
                    2 * ((d - 1) % 2) + i,
                    lax.rem(g + groups - sign * d, groups) * CHIPS + 2 * odd + i,
                    lax.rem(groups + sign * d, groups),
                )
        if k == 1:
            back(2, lax.rem(g + half, groups) * CHIPS + lax.rem(p + 2, CHIPS), half)
            pltpu.make_async_copy(obuf.at[k, 3], ret.at[0], r4).start()

    for cp in weight_copies:
        cp.wait()
    phases = {"H": hear, "D": dispatch, "W": dispatched, "S": select, "E": expert, "C": combine}
    for step in ORDER:
        phases[step[0]](int(step[1]))

    pltpu.make_async_copy(ret, ret, r4).wait()
    mixed = dot(unplace, ret[...].reshape(groups * SLOTS, width))
    for i in range(tp_count):
        mx[i] = mixed[:, i * piece:(i + 1) * piece].astype(BF16)
    mine = pltpu.make_async_copy(mx.at[t], out.at[pl.ds(t * rows, rows)], in_sem.at[2])
    mine.start()
    if tp_count > 1:
        @pl.loop(1, tp_count)
        def _(k):
            peer = lax.rem(t + k, tp_count)
            pltpu.make_async_remote_copy(
                src_ref=mx.at[peer], dst_ref=out.at[pl.ds(t * rows, rows)],
                send_sem=fin_send, recv_sem=fin_recv, device_id={"tp": peer}, device_id_type=MESH,
            ).start()

        others = mx.at[pl.ds(0, tp_count - 1)]
        pltpu.make_async_copy(others, others, fin_recv).wait()
        pltpu.make_async_copy(others, others, fin_send).wait()
        others = xin.at[pl.ds(0, tp_count - 1)]
        pltpu.make_async_copy(others, others, tp_send).wait()
    mine.wait()

    for k in range(NB):
        if "W%d" % k not in ORDER:
            dispatched(k)
    for src, sem in ((sbuf, s2), (yo, s3)):
        every = src.at[:, pl.ds(0, EPG - 1)]
        pltpu.make_async_copy(every, every, sem).wait()
    every = ret.at[pl.ds(0, groups - 1)]
    pltpu.make_async_copy(every, every, s4).wait()


def local(tokens, norm_gain, gate_weight, up_weight, down_weight, expert_ids, route_weight, ep_count, tp_count):
    tok, piece = tokens.shape
    rows = tok // tp_count
    _, width, ff = gate_weight.shape
    groups = ep_count // EPG
    nb = NB
    wide = width + 128
    any_spec = pl.BlockSpec(memory_space=pl.ANY)
    dma = pltpu.SemaphoreType.DMA
    return pl.pallas_call(
        partial(body, ep_count, tp_count),
        out_shape=jax.ShapeDtypeStruct(tokens.shape, BF16),
        in_specs=[any_spec] * 7,
        out_specs=any_spec,
        scratch_shapes=[
            pltpu.VMEM((tok, piece), BF16),
            pltpu.VMEM((tp_count, rows, piece), BF16),
            pltpu.VMEM((1, width), F32),
            pltpu.VMEM((2, tok), jnp.int32),
            pltpu.VMEM((2, tok), F32),
            pltpu.VMEM((width, ff), BF16),
            pltpu.VMEM((width, ff), BF16),
            pltpu.VMEM((ff, width), BF16),
            pltpu.VMEM((rows, wide), BF16),
            pltpu.VMEM((groups, SLOTS, wide), BF16),
            pltpu.VMEM((nb, 4, SLOTS, wide), BF16),
            pltpu.VMEM((nb, EPG, 8, width), BF16),
            pltpu.VMEM((nb, EPG, 8, width), BF16),
            pltpu.VMEM((nb, EPG, 8, width), BF16),
            pltpu.VMEM((nb, EPG, 8, width), BF16),
            pltpu.VMEM((nb, 4, SLOTS, width), BF16),
            pltpu.VMEM((groups, SLOTS, width), BF16),
            pltpu.VMEM((tp_count, rows, piece), BF16),
            pltpu.SemaphoreType.REGULAR((8,)),
            dma((3,)), dma((4,)), dma, dma,
            dma((nb,)), dma((nb,)), dma, dma((nb,)), dma, dma((nb,)), dma, dma, dma, dma,
        ],
        compiler_params=pltpu.CompilerParams(
            collective_id=0, has_side_effects=True, vmem_limit_bytes=67043328
        ),
        name="moe",
    )(tokens, norm_gain.reshape(1, width), gate_weight, up_weight, down_weight, expert_ids.T, route_weight.T)


def solution(mesh):
    in_specs = (
        P("ep", "tp"),
        P(),
        P("ep", None, None),
        P("ep", None, None),
        P("ep", None, None),
        P("ep", None),
        P("ep", None),
    )
    fn = partial(local, ep_count=mesh.shape["ep"], tp_count=mesh.shape["tp"])
    return jax.shard_map(fn, mesh=mesh, in_specs=in_specs, out_specs=P("ep", "tp"), check_vma=False)
```

```python
from functools import partial

import jax
import jax.numpy as jnp
from jax import lax
from jax.experimental import pallas as pl
from jax.experimental.pallas import tpu as pltpu
from jax.sharding import PartitionSpec as P

MESH = pl.DeviceIdType.MESH
F32 = jnp.float32
BF16 = jnp.bfloat16
CHIPS = 4
EPG = 8
SLOTS = 8
ORDER = ('D0', 'H3', 'D1', 'S0', 'S1', 'E0', 'E1', 'C0', 'A0', 'C1', 'A1', 'X1', 'X0')
RETURNS = {
    'A0': ((0,), 0, 4, True),
    'A1': ((1,), 0, 4, True),
    'B0': ((0,), 4, 12, True),
    'B1': ((1,), 4, 12, True),
    'G0': ((0,), 12, 32, True),
    'G1': ((1,), 12, 32, True),
    'W': ((0, 1), 0, 32, False),
    'X0': ((0,), 4, 32, True),
    'X1': ((1,), 4, 32, True),
}
NB = 2
HOPS = (1, 2, 4, 6)


def dot(a, b, contract=((1,), (0,))):
    return lax.dot_general(a, b, (contract, ((), ())), preferred_element_type=F32)


def to_row(col):
    n = col.shape[0]
    eye = lax.broadcasted_iota(jnp.int32, (n, n), 0) == lax.broadcasted_iota(jnp.int32, (n, n), 1)
    return jnp.sum(jnp.where(eye, col, jnp.zeros_like(col)), axis=0, keepdims=True)


def body(
    ep_count, tp_count,
    tokens, gain_hbm, gate_hbm, up_hbm, down_hbm, ids_hbm, wts_hbm,
    out,
    tok_v, xin, gain, ids, wts, gate, up, down, xn, sb, rbuf, sbuf, xe, yo, pbuf, obuf, ret, mx,
    known, w_sem, in_sem, tp_send, tp_recv, s1, r1, s2, r2, s3, r3, s4, r4, fin_send, fin_recv,
):
    e = lax.axis_index("ep")
    t = lax.axis_index("tp")
    groups = ep_count // EPG
    chips = ep_count // 2
    half = groups // 2
    c = lax.rem(e, 2)
    z = e // 2
    p = lax.rem(z, CHIPS)
    g = z // CHIPS
    rows = xn.shape[0]
    width = gate.shape[0]
    my_e = 2 * p + c

    weight_copies = [
        pltpu.make_async_copy(gate_hbm.at[0], gate, w_sem.at[0]),
        pltpu.make_async_copy(up_hbm.at[0], up, w_sem.at[1]),
        pltpu.make_async_copy(down_hbm.at[0], down, w_sem.at[2]),
    ]
    small_copies = [
        pltpu.make_async_copy(ids_hbm, ids, in_sem.at[0]),
        pltpu.make_async_copy(wts_hbm, wts, in_sem.at[1]),
        pltpu.make_async_copy(tokens, tok_v, in_sem.at[2]),
        pltpu.make_async_copy(gain_hbm, gain, in_sem.at[3]),
    ]
    for cp in small_copies:
        cp.start()
    barrier = pltpu.get_barrier_semaphore()

    def column(zz):
        return {"ep": lax.rem(zz + 2 * chips, chips) * 2 + c}

    for peer in ({"ep": z * 2 + 1 - c}, column(z + 1), column(z - 1)):
        pl.semaphore_signal(barrier, inc=1, device_id=peer, device_id_type=MESH)

    if tp_count > 1:
        @pl.loop(1, tp_count)
        def _(k):
            pl.semaphore_signal(barrier, inc=1, device_id={"tp": lax.rem(t + k, tp_count)}, device_id_type=MESH)

    for cp in weight_copies:
        cp.start()

    for cp in small_copies[:2]:
        cp.wait()
    tok = ids.shape[1]
    pick = lax.broadcasted_iota(jnp.int32, (rows, tok), 1) == (
        lax.broadcasted_iota(jnp.int32, (rows, tok), 0) + t * rows
    )
    id_col = [jnp.sum(jnp.where(pick, ids[k:k + 1, :], 0), axis=1, keepdims=True) for k in range(2)]
    w_col = [jnp.sum(jnp.where(pick, wts[k:k + 1, :], 0.0), axis=1, keepdims=True) for k in range(2)]
    id_row = [to_row(v) for v in id_col]
    before = lax.broadcasted_iota(jnp.int32, (rows, rows), 1) < lax.broadcasted_iota(jnp.int32, (rows, rows), 0)
    g_col = id_col[0] // EPG
    same = before & ((id_row[0] // EPG) == g_col)
    rank = jnp.sum(jnp.where(same, 1, 0), axis=1, keepdims=True)
    rel = lax.rem(g_col - g + groups, groups)
    target = rel * SLOTS + rank
    q_col = []
    for k in range(2):
        hit = jnp.where(id_row[0] == id_col[k], 1, 0) + jnp.where(id_row[1] == id_col[k], 1, 0)
        q_col.append(jnp.sum(jnp.where(before, hit, 0), axis=1, keepdims=True))
    lane = lax.broadcasted_iota(jnp.int32, (rows, 128), 1)
    lane_lo = lax.rem(lane, 64)
    w_tok = jnp.zeros((rows, 128), F32)
    for k in range(2):
        high = w_col[k].astype(BF16).astype(F32)
        part = jnp.where(lane < 64, high, w_col[k] - high)
        on = (lane_lo // 8 == lax.rem(id_col[k], EPG)) & (lax.rem(lane, 2) == q_col[k])
        w_tok = w_tok + jnp.where(on, part, 0.0)
    xn[:, width:] = w_tok.astype(BF16)
    place = jnp.where(
        lax.broadcasted_iota(jnp.int32, (groups * SLOTS, rows), 0) == to_row(target), 1.0, 0.0
    ).astype(BF16)
    unplace = jnp.where(
        lax.broadcasted_iota(jnp.int32, (rows, groups * SLOTS), 1) == target, 1.0, 0.0
    ).astype(BF16)

    for cp in small_copies[2:]:
        cp.wait()
    xin[t] = tok_v[pl.ds(pl.multiple_of(t * rows, rows), rows), :]
    pl.semaphore_wait(barrier, 3 + (tp_count - 1))

    if tp_count > 1:
        @pl.loop(1, tp_count)
        def _(k):
            peer = lax.rem(t + k, tp_count)
            pltpu.make_async_remote_copy(
                src_ref=tok_v.at[pl.ds(peer * rows, rows)], dst_ref=xin.at[t],
                send_sem=tp_send, recv_sem=tp_recv, device_id={"tp": peer}, device_id_type=MESH,
            ).start()

    def tell(i):
        for side in range(2):
            pl.semaphore_signal(
                known.at[2 * i + side], inc=1, device_id=column(z + (1 - 2 * side) * HOPS[i]), device_id_type=MESH
            )

    def hear(i):
        for side in range(2):
            pl.semaphore_wait(known.at[2 * i + side], 1)

    for i in range(3):
        tell(i)
        hear(i)
    tell(3)
    if tp_count > 1:
        pltpu.make_async_copy(xin.at[pl.ds(0, tp_count - 1)], xin.at[pl.ds(0, tp_count - 1)], tp_recv).wait()
    piece = xin.shape[2]
    total = jnp.zeros((rows, piece), F32)
    for i in range(tp_count):
        v = xin[i].astype(F32)
        total = total + v * v
    scale = lax.rsqrt(jnp.sum(total, axis=1, keepdims=True) / width + 1e-06)
    for i in range(tp_count):
        cols = slice(i * piece, (i + 1) * piece)
        xn[:, cols] = (xin[i].astype(F32) * scale * gain[:, cols]).astype(BF16)
    placed = dot(place, xn[...])
    for r in range(groups):
        sb[r] = placed[r * SLOTS:(r + 1) * SLOTS].astype(BF16)

    def ep_of(zz):
        return {"ep": zz * 2 + c}

    def send1(r, dest_z, k, b):
        return pltpu.make_async_remote_copy(
            src_ref=sb.at[r], dst_ref=rbuf.at[k, b], send_sem=s1.at[k], recv_sem=r1.at[k],
            device_id=ep_of(dest_z), device_id_type=MESH,
        )

    odd = lax.rem(p, 2)
    top = p // 2
    peers = [2 * chip + core for chip in (3 * (1 - top), 2 - top, 1 + 4 * top - p) for core in (0, 1)]
    peers.append(my_e + 1 - 2 * c)

    def dispatch(k):
        if k == 1:
            send1(half, lax.rem(g + half, groups) * CHIPS + 2 * (1 - p // 2) + odd, k, 2).start()
            pltpu.make_async_copy(sb.at[0], rbuf.at[k, 3], r1.at[k]).start()
        for d in (2, 1) if k == 0 else (3,):
            b = 2 * ((d - 1) % 2) + odd
            send1(d, lax.rem(g + d, groups) * CHIPS + p // 2, k, b).start()
            send1(groups - d, lax.rem(g + groups - d, groups) * CHIPS + 2 + p // 2, k, b).start()

    def dispatched(k):
        n = 4 if k == 0 else 3
        pltpu.make_async_copy(sb.at[pl.ds(0, n)], sb.at[pl.ds(0, n)], s1.at[k]).wait()

    row_of = lax.broadcasted_iota(jnp.int32, (32, 64), 0) // SLOTS
    lane_of = lax.rem(lax.broadcasted_iota(jnp.int32, (32, 64), 1) // 2, 4)
    diagonal = row_of == lane_of

    def select(k):
        pltpu.make_async_copy(rbuf.at[k], rbuf.at[k], r1.at[k]).wait()
        got = rbuf[k].reshape(4 * SLOTS, width + 128)
        wide = got[:, width:width + 64].astype(F32)
        sel = jnp.where(diagonal & (wide != 0.0), 1.0, 0.0).astype(BF16)
        chosen = dot(sel, got[:, :width], ((0,), (0,)))
        for ee in range(EPG):
            sbuf[k, ee] = chosen[ee * 8:(ee + 1) * 8].astype(BF16)
        for ee in peers:
            pltpu.make_async_remote_copy(
                src_ref=sbuf.at[k, ee], dst_ref=xe.at[k, my_e], send_sem=s2, recv_sem=r2.at[k],
                device_id={"ep": g * EPG + ee}, device_id_type=MESH,
            ).start()
        pltpu.make_async_copy(sbuf.at[k, my_e], xe.at[k, my_e], r2.at[k]).start()

    def expert(k):
        pltpu.make_async_copy(xe.at[k], xe.at[k], r2.at[k]).wait()
        x = xe[k].reshape(64, width)
        a = dot(x, gate[...])
        b = dot(x, up[...])
        h = (a / (1.0 + jnp.exp(-a)) * b).astype(BF16)
        y = dot(h, down[...])
        for i in range(EPG):
            yo[k, i] = y[i * 8:(i + 1) * 8].astype(BF16)
        for ee in peers:
            pltpu.make_async_remote_copy(
                src_ref=yo.at[k, ee], dst_ref=pbuf.at[k, my_e], send_sem=s3, recv_sem=r3.at[k],
                device_id={"ep": g * EPG + ee}, device_id_type=MESH,
            ).start()
        pltpu.make_async_copy(yo.at[k, my_e], pbuf.at[k, my_e], r3.at[k]).start()

    def combine(k):
        pltpu.make_async_copy(pbuf.at[k], pbuf.at[k], r3.at[k]).wait()
        parts = pbuf[k].reshape(64, width)
        wide = rbuf[k].reshape(4 * SLOTS, width + 128)[:, width:].astype(F32)
        high = jnp.where(diagonal, wide[:, :64], 0.0).astype(BF16)
        low = jnp.where(diagonal, wide[:, 64:], 0.0).astype(BF16)
        y = dot(high, parts) + dot(low, parts)
        for b in range(4):
            obuf[k, b] = y[b * 8:(b + 1) * 8].astype(BF16)
        if k == 1:
            pltpu.make_async_copy(obuf.at[k, 3], ret.at[0], r4).start()

    def returns():
        sign = 1 - 2 * (p // 2)
        found = []
        for d in (1, 2, 3):
            for i in range(2):
                src_z = lax.rem(g + groups - sign * d, groups) * CHIPS + 2 * odd + i
                found.append(((d - 1) // 2, 2 * ((d - 1) % 2) + i, src_z, lax.rem(groups + sign * d, groups)))
        found.append((1, 2, lax.rem(g + half, groups) * CHIPS + lax.rem(p + 2, CHIPS), half))
        return found

    def give(name):
        ks, low, high, act = RETURNS[name]
        for k, b, src_z, r in returns():
            if k in ks:
                @pl.when((src_z >= low) & (src_z < high))
                def _():
                    cp = pltpu.make_async_remote_copy(
                        src_ref=obuf.at[k, b], dst_ref=ret.at[r], send_sem=s4.at[k, b], recv_sem=r4,
                        device_id=ep_of(src_z), device_id_type=MESH,
                    )
                    if act:
                        cp.start()
                    else:
                        cp.wait_send()

    for cp in weight_copies:
        cp.wait()
    phases = {"H": hear, "D": dispatch, "W": dispatched, "S": select, "E": expert, "C": combine}
    for step in ORDER:
        if step in RETURNS:
            give(step)
        else:
            phases[step[0]](int(step[1]))

    pltpu.make_async_copy(ret, ret, r4).wait()
    mixed = dot(unplace, ret[...].reshape(groups * SLOTS, width))
    for i in range(tp_count):
        mx[i] = mixed[:, i * piece:(i + 1) * piece].astype(BF16)
    mine = pltpu.make_async_copy(mx.at[t], out.at[pl.ds(t * rows, rows)], in_sem.at[2])
    mine.start()
    if tp_count > 1:
        @pl.loop(1, tp_count)
        def _(k):
            peer = lax.rem(t + k, tp_count)
            pltpu.make_async_remote_copy(
                src_ref=mx.at[peer], dst_ref=out.at[pl.ds(t * rows, rows)],
                send_sem=fin_send, recv_sem=fin_recv, device_id={"tp": peer}, device_id_type=MESH,
            ).start()

        others = mx.at[pl.ds(0, tp_count - 1)]
        pltpu.make_async_copy(others, others, fin_recv).wait()
        pltpu.make_async_copy(others, others, fin_send).wait()
        others = xin.at[pl.ds(0, tp_count - 1)]
        pltpu.make_async_copy(others, others, tp_send).wait()
    mine.wait()

    for k in range(NB):
        if "W%d" % k not in ORDER:
            dispatched(k)
    give("W")
    for src, sem in ((sbuf, s2), (yo, s3)):
        every = src.at[:, pl.ds(0, EPG - 1)]
        pltpu.make_async_copy(every, every, sem).wait()


def local(tokens, norm_gain, gate_weight, up_weight, down_weight, expert_ids, route_weight, ep_count, tp_count):
    tok, piece = tokens.shape
    rows = tok // tp_count
    _, width, ff = gate_weight.shape
    groups = ep_count // EPG
    nb = NB
    wide = width + 128
    any_spec = pl.BlockSpec(memory_space=pl.ANY)
    dma = pltpu.SemaphoreType.DMA
    return pl.pallas_call(
        partial(body, ep_count, tp_count),
        out_shape=jax.ShapeDtypeStruct(tokens.shape, BF16),
        in_specs=[any_spec] * 7,
        out_specs=any_spec,
        scratch_shapes=[
            pltpu.VMEM((tok, piece), BF16),
            pltpu.VMEM((tp_count, rows, piece), BF16),
            pltpu.VMEM((1, width), F32),
            pltpu.VMEM((2, tok), jnp.int32),
            pltpu.VMEM((2, tok), F32),
            pltpu.VMEM((width, ff), BF16),
            pltpu.VMEM((width, ff), BF16),
            pltpu.VMEM((ff, width), BF16),
            pltpu.VMEM((rows, wide), BF16),
            pltpu.VMEM((groups, SLOTS, wide), BF16),
            pltpu.VMEM((nb, 4, SLOTS, wide), BF16),
            pltpu.VMEM((nb, EPG, 8, width), BF16),
            pltpu.VMEM((nb, EPG, 8, width), BF16),
            pltpu.VMEM((nb, EPG, 8, width), BF16),
            pltpu.VMEM((nb, EPG, 8, width), BF16),
            pltpu.VMEM((nb, 4, SLOTS, width), BF16),
            pltpu.VMEM((groups, SLOTS, width), BF16),
            pltpu.VMEM((tp_count, rows, piece), BF16),
            pltpu.SemaphoreType.REGULAR((8,)),
            dma((3,)), dma((4,)), dma, dma,
            dma((nb,)), dma((nb,)), dma, dma((nb,)), dma, dma((nb,)), dma((nb, 4)), dma, dma, dma,
        ],
        compiler_params=pltpu.CompilerParams(
            collective_id=0, has_side_effects=True, vmem_limit_bytes=67043328
        ),
        name="moe",
    )(tokens, norm_gain.reshape(1, width), gate_weight, up_weight, down_weight, expert_ids.T, route_weight.T)


def solution(mesh):
    in_specs = (
        P("ep", "tp"),
        P(),
        P("ep", None, None),
        P("ep", None, None),
        P("ep", None, None),
        P("ep", None),
        P("ep", None),
    )
    fn = partial(local, ep_count=mesh.shape["ep"], tp_count=mesh.shape["tp"])
    return jax.shard_map(fn, mesh=mesh, in_specs=in_specs, out_specs=P("ep", "tp"), check_vma=False)
```

```python
from functools import partial

import jax
import jax.numpy as jnp
from jax import lax
from jax.experimental import pallas as pl
from jax.experimental.pallas import tpu as pltpu
from jax.sharding import PartitionSpec as P

MESH = pl.DeviceIdType.MESH
F32 = jnp.float32
BF16 = jnp.bfloat16
CHIPS = 4
EPG = 8
SLOTS = 8
ORDER = ('D0', 'H3', 'D1', 'S0', 'S1', 'E0', 'E1', 'C0', 'A0', 'C1', 'A1', 'X1', 'X0')
RETURNS = {
    'A0': ((0,), 0, 4, True),
    'A1': ((1,), 0, 4, True),
    'B0': ((0,), 4, 12, True),
    'B1': ((1,), 4, 12, True),
    'G0': ((0,), 12, 32, True),
    'G1': ((1,), 12, 32, True),
    'W': ((0, 1), 0, 32, False),
    'X0': ((0,), 4, 32, True),
    'X1': ((1,), 4, 32, True),
}
NB = 2
HOPS = (1, 2, 4, 6)


def dot(a, b, contract=((1,), (0,))):
    return lax.dot_general(a, b, (contract, ((), ())), preferred_element_type=F32)


def to_row(col):
    n = col.shape[0]
    eye = lax.broadcasted_iota(jnp.int32, (n, n), 0) == lax.broadcasted_iota(jnp.int32, (n, n), 1)
    return jnp.sum(jnp.where(eye, col, jnp.zeros_like(col)), axis=0, keepdims=True)


def body(
    ep_count, tp_count,
    tokens, gain_hbm, gate_hbm, up_hbm, down_hbm, ids_hbm, wts_hbm,
    out,
    tok_v, xin, gain, ids, wts, gate, up, down, xn, sb, rbuf, sbuf, xe, yo, pbuf, obuf, ret, mx,
    wsend, wrecv, wmat, known, sw, rw, w_sem, in_sem, tp_send, tp_recv, s1, r1, s2, r2, s3, r3, s4, r4, fin_send, fin_recv,
):
    e = lax.axis_index("ep")
    t = lax.axis_index("tp")
    groups = ep_count // EPG
    chips = ep_count // 2
    half = groups // 2
    c = lax.rem(e, 2)
    z = e // 2
    p = lax.rem(z, CHIPS)
    g = z // CHIPS
    rows = xn.shape[0]
    width = gate.shape[0]
    my_e = 2 * p + c

    weight_copies = [
        pltpu.make_async_copy(gate_hbm.at[0], gate, w_sem.at[0]),
        pltpu.make_async_copy(up_hbm.at[0], up, w_sem.at[1]),
        pltpu.make_async_copy(down_hbm.at[0], down, w_sem.at[2]),
    ]
    small_copies = [
        pltpu.make_async_copy(ids_hbm, ids, in_sem.at[0]),
        pltpu.make_async_copy(wts_hbm, wts, in_sem.at[1]),
        pltpu.make_async_copy(tokens, tok_v, in_sem.at[2]),
        pltpu.make_async_copy(gain_hbm, gain, in_sem.at[3]),
    ]
    for cp in small_copies:
        cp.start()
    barrier = pltpu.get_barrier_semaphore()

    def column(zz):
        return {"ep": lax.rem(zz + 2 * chips, chips) * 2 + c}

    for peer in ({"ep": z * 2 + 1 - c}, column(z + 1), column(z - 1)):
        pl.semaphore_signal(barrier, inc=1, device_id=peer, device_id_type=MESH)

    if tp_count > 1:
        @pl.loop(1, tp_count)
        def _(k):
            pl.semaphore_signal(barrier, inc=1, device_id={"tp": lax.rem(t + k, tp_count)}, device_id_type=MESH)

    for cp in weight_copies:
        cp.start()

    for cp in small_copies[:2]:
        cp.wait()
    tok = ids.shape[1]
    pick = lax.broadcasted_iota(jnp.int32, (rows, tok), 1) == (
        lax.broadcasted_iota(jnp.int32, (rows, tok), 0) + t * rows
    )
    id_col = [jnp.sum(jnp.where(pick, ids[k:k + 1, :], 0), axis=1, keepdims=True) for k in range(2)]
    w_col = [jnp.sum(jnp.where(pick, wts[k:k + 1, :], 0.0), axis=1, keepdims=True) for k in range(2)]
    id_row = [to_row(v) for v in id_col]
    before = lax.broadcasted_iota(jnp.int32, (rows, rows), 1) < lax.broadcasted_iota(jnp.int32, (rows, rows), 0)
    g_col = id_col[0] // EPG
    same = before & ((id_row[0] // EPG) == g_col)
    rank = jnp.sum(jnp.where(same, 1, 0), axis=1, keepdims=True)
    rel = lax.rem(g_col - g + groups, groups)
    target = rel * SLOTS + rank
    q_col = []
    for k in range(2):
        hit = jnp.where(id_row[0] == id_col[k], 1, 0) + jnp.where(id_row[1] == id_col[k], 1, 0)
        q_col.append(jnp.sum(jnp.where(before, hit, 0), axis=1, keepdims=True))
    lane = lax.broadcasted_iota(jnp.int32, (rows, 128), 1)
    w_tok = jnp.zeros((rows, 128), F32)
    for k in range(2):
        on = lane == rank * 16 + lax.rem(id_col[k], EPG) * 2 + q_col[k]
        w_tok = w_tok + jnp.where(on, w_col[k], 0.0)
    w_high = w_tok.astype(BF16)
    w_low = (w_tok - w_high.astype(F32)).astype(BF16)
    of_group = jnp.where(
        lax.broadcasted_iota(jnp.int32, (groups, rows), 0) == to_row(rel), 1.0, 0.0
    ).astype(BF16)
    table = dot(of_group, w_high) + dot(of_group, w_low)
    for r in range(groups):
        wsend[r] = table[r:r + 1]
    place = jnp.where(
        lax.broadcasted_iota(jnp.int32, (groups * SLOTS, rows), 0) == to_row(target), 1.0, 0.0
    ).astype(BF16)
    unplace = jnp.where(
        lax.broadcasted_iota(jnp.int32, (rows, groups * SLOTS), 1) == target, 1.0, 0.0
    ).astype(BF16)

    for cp in small_copies[2:]:
        cp.wait()
    xin[t] = tok_v[pl.ds(pl.multiple_of(t * rows, rows), rows), :]
    pl.semaphore_wait(barrier, 3 + (tp_count - 1))

    if tp_count > 1:
        @pl.loop(1, tp_count)
        def _(k):
            peer = lax.rem(t + k, tp_count)
            pltpu.make_async_remote_copy(
                src_ref=tok_v.at[pl.ds(peer * rows, rows)], dst_ref=xin.at[t],
                send_sem=tp_send, recv_sem=tp_recv, device_id={"tp": peer}, device_id_type=MESH,
            ).start()

    def tell(i):
        for side in range(2):
            pl.semaphore_signal(
                known.at[2 * i + side], inc=1, device_id=column(z + (1 - 2 * side) * HOPS[i]), device_id_type=MESH
            )

    def hear(i):
        for side in range(2):
            pl.semaphore_wait(known.at[2 * i + side], 1)

    for i in range(3):
        tell(i)
        hear(i)
    tell(3)
    if tp_count > 1:
        pltpu.make_async_copy(xin.at[pl.ds(0, tp_count - 1)], xin.at[pl.ds(0, tp_count - 1)], tp_recv).wait()
    piece = xin.shape[2]
    total = jnp.zeros((rows, piece), F32)
    for i in range(tp_count):
        v = xin[i].astype(F32)
        total = total + v * v
    scale = lax.rsqrt(jnp.sum(total, axis=1, keepdims=True) / width + 1e-06)
    for i in range(tp_count):
        cols = slice(i * piece, (i + 1) * piece)
        xn[:, cols] = (xin[i].astype(F32) * scale * gain[:, cols]).astype(BF16)
    placed = dot(place, xn[...])
    for r in range(groups):
        sb[r] = placed[r * SLOTS:(r + 1) * SLOTS].astype(BF16)

    def ep_of(zz):
        return {"ep": zz * 2 + c}

    def send1(r, dest_z, k, b):
        return pltpu.make_async_remote_copy(
            src_ref=sb.at[r], dst_ref=rbuf.at[k, b], send_sem=s1.at[k], recv_sem=r1.at[k],
            device_id=ep_of(dest_z), device_id_type=MESH,
        )

    def sendw(r, dest_z, k, b):
        return pltpu.make_async_remote_copy(
            src_ref=wsend.at[r], dst_ref=wrecv.at[k, b], send_sem=sw.at[k], recv_sem=rw.at[k],
            device_id=ep_of(dest_z), device_id_type=MESH,
        )

    odd = lax.rem(p, 2)
    top = p // 2
    peers = [2 * chip + core for chip in (3 * (1 - top), 2 - top, 1 + 4 * top - p) for core in (0, 1)]
    peers.append(my_e + 1 - 2 * c)

    def dispatch(k):
        plan = []
        if k == 1:
            plan.append((half, lax.rem(g + half, groups) * CHIPS + 2 * (1 - p // 2) + odd, 2))
            pltpu.make_async_copy(sb.at[0], rbuf.at[k, 3], r1.at[k]).start()
            pltpu.make_async_copy(wsend.at[0], wrecv.at[k, 3], rw.at[k]).start()
        for d in (2, 1) if k == 0 else (3,):
            b = 2 * ((d - 1) % 2) + odd
            plan.append((d, lax.rem(g + d, groups) * CHIPS + p // 2, b))
            plan.append((groups - d, lax.rem(g + groups - d, groups) * CHIPS + 2 + p // 2, b))
        for send in (sendw, send1):
            for r, dest_z, b in plan:
                send(r, dest_z, k, b).start()

    def dispatched(k):
        n = 4 if k == 0 else 3
        pltpu.make_async_copy(sb.at[pl.ds(0, n)], sb.at[pl.ds(0, n)], s1.at[k]).wait()
        pltpu.make_async_copy(wsend.at[pl.ds(0, n)], wsend.at[pl.ds(0, n)], sw.at[k]).wait()

    row_of = lax.broadcasted_iota(jnp.int32, (32, 64), 0) // SLOTS
    lane_of = lax.rem(lax.broadcasted_iota(jnp.int32, (32, 64), 1) // 2, 4)
    diagonal = row_of == lane_of
    slot_of = lax.rem(lax.broadcasted_iota(jnp.int32, (32, 128), 0), SLOTS)
    in_slot = lax.broadcasted_iota(jnp.int32, (32, 128), 1) // 16 == slot_of
    wide_row = lax.rem(lax.broadcasted_iota(jnp.int32, (128, 64), 0), 16)
    wide_lane = lax.broadcasted_iota(jnp.int32, (128, 64), 1)
    spread = jnp.where(wide_row == wide_lane // 8 * 2 + lax.rem(wide_lane, 2), 1.0, 0.0).astype(BF16)

    def select(k):
        pltpu.make_async_copy(rbuf.at[k], rbuf.at[k], r1.at[k]).wait()
        pltpu.make_async_copy(wrecv.at[k], wrecv.at[k], rw.at[k]).wait()
        weights = jnp.concatenate([jnp.broadcast_to(wrecv[k, b], (SLOTS, 128)) for b in range(4)], axis=0)
        weights = jnp.where(in_slot, weights, 0.0)
        w_hi = weights.astype(BF16)
        w_lo = (weights - w_hi.astype(F32)).astype(BF16)
        high = jnp.where(diagonal, dot(w_hi, spread), 0.0)
        low = jnp.where(diagonal, dot(w_lo, spread), 0.0)
        wmat[k, 0] = high.astype(BF16)
        wmat[k, 1] = low.astype(BF16)
        sel = jnp.where(high != 0.0, 1.0, 0.0).astype(BF16)
        chosen = dot(sel, rbuf[k].reshape(4 * SLOTS, width), ((0,), (0,)))
        for ee in range(EPG):
            sbuf[k, ee] = chosen[ee * 8:(ee + 1) * 8].astype(BF16)
        for ee in peers:
            pltpu.make_async_remote_copy(
                src_ref=sbuf.at[k, ee], dst_ref=xe.at[k, my_e], send_sem=s2, recv_sem=r2.at[k],
                device_id={"ep": g * EPG + ee}, device_id_type=MESH,
            ).start()
        pltpu.make_async_copy(sbuf.at[k, my_e], xe.at[k, my_e], r2.at[k]).start()

    def expert(k):
        pltpu.make_async_copy(xe.at[k], xe.at[k], r2.at[k]).wait()
        x = xe[k].reshape(64, width)
        a = dot(x, gate[...])
        b = dot(x, up[...])
        h = (a / (1.0 + jnp.exp(-a)) * b).astype(BF16)
        y = dot(h, down[...])
        for i in range(EPG):
            yo[k, i] = y[i * 8:(i + 1) * 8].astype(BF16)
        for ee in peers:
            pltpu.make_async_remote_copy(
                src_ref=yo.at[k, ee], dst_ref=pbuf.at[k, my_e], send_sem=s3, recv_sem=r3.at[k],
                device_id={"ep": g * EPG + ee}, device_id_type=MESH,
            ).start()
        pltpu.make_async_copy(yo.at[k, my_e], pbuf.at[k, my_e], r3.at[k]).start()

    def combine(k):
        pltpu.make_async_copy(pbuf.at[k], pbuf.at[k], r3.at[k]).wait()
        parts = pbuf[k].reshape(64, width)
        y = dot(wmat[k, 0], parts) + dot(wmat[k, 1], parts)
        for b in range(4):
            obuf[k, b] = y[b * 8:(b + 1) * 8].astype(BF16)
        if k == 1:
            pltpu.make_async_copy(obuf.at[k, 3], ret.at[0], r4).start()

    def returns():
        sign = 1 - 2 * (p // 2)
        found = []
        for d in (1, 2, 3):
            for i in range(2):
                src_z = lax.rem(g + groups - sign * d, groups) * CHIPS + 2 * odd + i
                found.append(((d - 1) // 2, 2 * ((d - 1) % 2) + i, src_z, lax.rem(groups + sign * d, groups)))
        found.append((1, 2, lax.rem(g + half, groups) * CHIPS + lax.rem(p + 2, CHIPS), half))
        return found

    def give(name):
        ks, low, high, act = RETURNS[name]
        for k, b, src_z, r in returns():
            if k in ks:
                @pl.when((src_z >= low) & (src_z < high))
                def _():
                    cp = pltpu.make_async_remote_copy(
                        src_ref=obuf.at[k, b], dst_ref=ret.at[r], send_sem=s4.at[k, b], recv_sem=r4,
                        device_id=ep_of(src_z), device_id_type=MESH,
                    )
                    if act:
                        cp.start()
                    else:
                        cp.wait_send()

    for cp in weight_copies:
        cp.wait()
    phases = {"H": hear, "D": dispatch, "W": dispatched, "S": select, "E": expert, "C": combine}
    for step in ORDER:
        if step in RETURNS:
            give(step)
        else:
            phases[step[0]](int(step[1]))

    pltpu.make_async_copy(ret, ret, r4).wait()
    mixed = dot(unplace, ret[...].reshape(groups * SLOTS, width))
    for i in range(tp_count):
        mx[i] = mixed[:, i * piece:(i + 1) * piece].astype(BF16)
    mine = pltpu.make_async_copy(mx.at[t], out.at[pl.ds(t * rows, rows)], in_sem.at[2])
    mine.start()
    if tp_count > 1:
        @pl.loop(1, tp_count)
        def _(k):
            peer = lax.rem(t + k, tp_count)
            pltpu.make_async_remote_copy(
                src_ref=mx.at[peer], dst_ref=out.at[pl.ds(t * rows, rows)],
                send_sem=fin_send, recv_sem=fin_recv, device_id={"tp": peer}, device_id_type=MESH,
            ).start()

        others = mx.at[pl.ds(0, tp_count - 1)]
        pltpu.make_async_copy(others, others, fin_recv).wait()
        pltpu.make_async_copy(others, others, fin_send).wait()
        others = xin.at[pl.ds(0, tp_count - 1)]
        pltpu.make_async_copy(others, others, tp_send).wait()
    mine.wait()

    for k in range(NB):
        if "W%d" % k not in ORDER:
            dispatched(k)
    give("W")
    for src, sem in ((sbuf, s2), (yo, s3)):
        every = src.at[:, pl.ds(0, EPG - 1)]
        pltpu.make_async_copy(every, every, sem).wait()


def local(tokens, norm_gain, gate_weight, up_weight, down_weight, expert_ids, route_weight, ep_count, tp_count):
    tok, piece = tokens.shape
    rows = tok // tp_count
    _, width, ff = gate_weight.shape
    groups = ep_count // EPG
    nb = NB
    any_spec = pl.BlockSpec(memory_space=pl.ANY)
    dma = pltpu.SemaphoreType.DMA
    return pl.pallas_call(
        partial(body, ep_count, tp_count),
        out_shape=jax.ShapeDtypeStruct(tokens.shape, BF16),
        in_specs=[any_spec] * 7,
        out_specs=any_spec,
        scratch_shapes=[
            pltpu.VMEM((tok, piece), BF16),
            pltpu.VMEM((tp_count, rows, piece), BF16),
            pltpu.VMEM((1, width), F32),
            pltpu.VMEM((2, tok), jnp.int32),
            pltpu.VMEM((2, tok), F32),
            pltpu.VMEM((width, ff), BF16),
            pltpu.VMEM((width, ff), BF16),
            pltpu.VMEM((ff, width), BF16),
            pltpu.VMEM((rows, width), BF16),
            pltpu.VMEM((groups, SLOTS, width), BF16),
            pltpu.VMEM((nb, 4, SLOTS, width), BF16),
            pltpu.VMEM((nb, EPG, 8, width), BF16),
            pltpu.VMEM((nb, EPG, 8, width), BF16),
            pltpu.VMEM((nb, EPG, 8, width), BF16),
            pltpu.VMEM((nb, EPG, 8, width), BF16),
            pltpu.VMEM((nb, 4, SLOTS, width), BF16),
            pltpu.VMEM((groups, SLOTS, width), BF16),
            pltpu.VMEM((tp_count, rows, piece), BF16),
            pltpu.VMEM((groups, 1, 128), F32),
            pltpu.VMEM((nb, 4, 1, 128), F32),
            pltpu.VMEM((nb, 2, 32, 64), BF16),
            pltpu.SemaphoreType.REGULAR((8,)),
            dma((nb,)), dma((nb,)),
            dma((3,)), dma((4,)), dma, dma,
            dma((nb,)), dma((nb,)), dma, dma((nb,)), dma, dma((nb,)), dma((nb, 4)), dma, dma, dma,
        ],
        compiler_params=pltpu.CompilerParams(
            collective_id=0, has_side_effects=True, vmem_limit_bytes=67043328
        ),
        name="moe",
    )(tokens, norm_gain.reshape(1, width), gate_weight, up_weight, down_weight, expert_ids.T, route_weight.T)


def solution(mesh):
    in_specs = (
        P("ep", "tp"),
        P(),
        P("ep", None, None),
        P("ep", None, None),
        P("ep", None, None),
        P("ep", None),
        P("ep", None),
    )
    fn = partial(local, ep_count=mesh.shape["ep"], tp_count=mesh.shape["tp"])
    return jax.shard_map(fn, mesh=mesh, in_specs=in_specs, out_specs=P("ep", "tp"), check_vma=False)
```

```python
from functools import partial

import jax
import jax.numpy as jnp
from jax import lax
from jax.experimental import pallas as pl
from jax.experimental.pallas import tpu as pltpu
from jax.sharding import PartitionSpec as P

MESH = pl.DeviceIdType.MESH
F32 = jnp.float32
BF16 = jnp.bfloat16
CHIPS = 4
PLANE = ((2, 2), (1, 2), (2, 1), (2, 3), (3, 2), (0, 2), (1, 1), (1, 3), (2, 0), (3, 1), (3, 3), (0, 1), (0, 3), (1, 0), (3, 0))
EPG = 8
SLOTS = 8
ORDER = ('D0', 'H3', 'D1', 'S0', 'S1', 'E0', 'E1', 'C0', 'A0', 'C1', 'A1', 'B1', 'B0', 'G1', 'G0')
RETURNS = {
    'A0': ((0,), 0, 4, True),
    'A1': ((1,), 0, 4, True),
    'B0': ((0,), 4, 10, True),
    'B1': ((1,), 4, 10, True),
    'G0': ((0,), 10, 32, True),
    'G1': ((1,), 10, 32, True),
    'W': ((0, 1), 0, 32, False),
}
NB = 2
HOPS = (1, 2, 4, 6)


def dot(a, b, contract=((1,), (0,))):
    return lax.dot_general(a, b, (contract, ((), ())), preferred_element_type=F32)


def to_row(col):
    n = col.shape[0]
    eye = lax.broadcasted_iota(jnp.int32, (n, n), 0) == lax.broadcasted_iota(jnp.int32, (n, n), 1)
    return jnp.sum(jnp.where(eye, col, jnp.zeros_like(col)), axis=0, keepdims=True)


def body(
    ep_count, tp_count,
    tokens, gain_hbm, gate_hbm, up_hbm, down_hbm, ids_hbm, wts_hbm,
    out,
    tok_v, xin, gain, ids, wts, gate, up, down, xn, sb, rbuf, sbuf, xe, yo, pbuf, obuf, ret, mx,
    wsend, wrecv, wmat, known, sw, rw, w_sem, in_sem, tp_send, tp_recv, s1, r1, s2, r2, s3, r3, s4, r4, fin_send, fin_recv,
):
    e = lax.axis_index("ep")
    t = lax.axis_index("tp")
    groups = ep_count // EPG
    chips = ep_count // 2
    half = groups // 2
    c = lax.rem(e, 2)
    z = e // 2
    p = lax.rem(z, CHIPS)
    g = z // CHIPS
    rows = xn.shape[0]
    width = gate.shape[0]
    my_e = 2 * p + c

    weight_copies = [
        pltpu.make_async_copy(gate_hbm.at[0], gate, w_sem.at[0]),
        pltpu.make_async_copy(up_hbm.at[0], up, w_sem.at[1]),
        pltpu.make_async_copy(down_hbm.at[0], down, w_sem.at[2]),
    ]
    small_copies = [
        pltpu.make_async_copy(ids_hbm, ids, in_sem.at[0]),
        pltpu.make_async_copy(wts_hbm, wts, in_sem.at[1]),
        pltpu.make_async_copy(tokens, tok_v, in_sem.at[2]),
        pltpu.make_async_copy(gain_hbm, gain, in_sem.at[3]),
    ]
    for cp in small_copies:
        cp.start()
    barrier = pltpu.get_barrier_semaphore()

    def column(zz):
        return {"ep": lax.rem(zz + 2 * chips, chips) * 2 + c}

    for peer in ({"ep": z * 2 + 1 - c}, column(z + 1), column(z - 1)):
        pl.semaphore_signal(barrier, inc=1, device_id=peer, device_id_type=MESH)

    if tp_count > 1:
        for dy, dx in PLANE:
            peer = lax.rem(t // CHIPS + dy, CHIPS) * CHIPS + lax.rem(t + dx, CHIPS)
            pl.semaphore_signal(barrier, inc=1, device_id={"tp": peer}, device_id_type=MESH)

    for cp in weight_copies:
        cp.start()

    for cp in small_copies[:2]:
        cp.wait()
    tok = ids.shape[1]
    pick = lax.broadcasted_iota(jnp.int32, (rows, tok), 1) == (
        lax.broadcasted_iota(jnp.int32, (rows, tok), 0) + t * rows
    )
    id_col = [jnp.sum(jnp.where(pick, ids[k:k + 1, :], 0), axis=1, keepdims=True) for k in range(2)]
    w_col = [jnp.sum(jnp.where(pick, wts[k:k + 1, :], 0.0), axis=1, keepdims=True) for k in range(2)]
    id_row = [to_row(v) for v in id_col]
    before = lax.broadcasted_iota(jnp.int32, (rows, rows), 1) < lax.broadcasted_iota(jnp.int32, (rows, rows), 0)
    g_col = id_col[0] // EPG
    same = before & ((id_row[0] // EPG) == g_col)
    rank = jnp.sum(jnp.where(same, 1, 0), axis=1, keepdims=True)
    rel = lax.rem(g_col - g + groups, groups)
    target = rel * SLOTS + rank
    q_col = []
    for k in range(2):
        hit = jnp.where(id_row[0] == id_col[k], 1, 0) + jnp.where(id_row[1] == id_col[k], 1, 0)
        q_col.append(jnp.sum(jnp.where(before, hit, 0), axis=1, keepdims=True))
    lane = lax.broadcasted_iota(jnp.int32, (rows, 128), 1)
    w_tok = jnp.zeros((rows, 128), F32)
    for k in range(2):
        on = lane == rank * 16 + lax.rem(id_col[k], EPG) * 2 + q_col[k]
        w_tok = w_tok + jnp.where(on, w_col[k], 0.0)
    w_high = w_tok.astype(BF16)
    w_low = (w_tok - w_high.astype(F32)).astype(BF16)
    of_group = jnp.where(
        lax.broadcasted_iota(jnp.int32, (groups, rows), 0) == to_row(rel), 1.0, 0.0
    ).astype(BF16)
    table = dot(of_group, w_high) + dot(of_group, w_low)
    for r in range(groups):
        wsend[r] = table[r:r + 1]
    place = jnp.where(
        lax.broadcasted_iota(jnp.int32, (groups * SLOTS, rows), 0) == to_row(target), 1.0, 0.0
    ).astype(BF16)
    unplace = jnp.where(
        lax.broadcasted_iota(jnp.int32, (rows, groups * SLOTS), 1) == target, 1.0, 0.0
    ).astype(BF16)

    for cp in small_copies[2:]:
        cp.wait()
    xin[t] = tok_v[pl.ds(pl.multiple_of(t * rows, rows), rows), :]
    pl.semaphore_wait(barrier, 3 + (tp_count - 1))

    if tp_count > 1:
        for dy, dx in PLANE:
            peer = lax.rem(t // CHIPS + dy, CHIPS) * CHIPS + lax.rem(t + dx, CHIPS)
            pltpu.make_async_remote_copy(
                src_ref=tok_v.at[pl.ds(peer * rows, rows)], dst_ref=xin.at[t],
                send_sem=tp_send, recv_sem=tp_recv, device_id={"tp": peer}, device_id_type=MESH,
            ).start()

    def tell(i):
        for side in range(2):
            pl.semaphore_signal(
                known.at[2 * i + side], inc=1, device_id=column(z + (1 - 2 * side) * HOPS[i]), device_id_type=MESH
            )

    def hear(i):
        for side in range(2):
            pl.semaphore_wait(known.at[2 * i + side], 1)

    for i in range(3):
        tell(i)
        hear(i)
    tell(3)
    if tp_count > 1:
        pltpu.make_async_copy(xin.at[pl.ds(0, tp_count - 1)], xin.at[pl.ds(0, tp_count - 1)], tp_recv).wait()
    piece = xin.shape[2]
    total = jnp.zeros((rows, piece), F32)
    for i in range(tp_count):
        v = xin[i].astype(F32)
        total = total + v * v
    scale = lax.rsqrt(jnp.sum(total, axis=1, keepdims=True) / width + 1e-06)
    for i in range(tp_count):
        cols = slice(i * piece, (i + 1) * piece)
        xn[:, cols] = (xin[i].astype(F32) * scale * gain[:, cols]).astype(BF16)
    placed = dot(place, xn[...])
    for r in range(groups):
        sb[r] = placed[r * SLOTS:(r + 1) * SLOTS].astype(BF16)

    def ep_of(zz):
        return {"ep": zz * 2 + c}

    def send1(r, dest_z, k, b):
        return pltpu.make_async_remote_copy(
            src_ref=sb.at[r], dst_ref=rbuf.at[k, b], send_sem=s1.at[k], recv_sem=r1.at[k],
            device_id=ep_of(dest_z), device_id_type=MESH,
        )

    def sendw(r, dest_z, k, b):
        return pltpu.make_async_remote_copy(
            src_ref=wsend.at[r], dst_ref=wrecv.at[k, b], send_sem=sw.at[k], recv_sem=rw.at[k],
            device_id=ep_of(dest_z), device_id_type=MESH,
        )

    odd = lax.rem(p, 2)
    top = p // 2
    peers = [2 * chip + core for chip in (3 * (1 - top), 2 - top, 1 + 4 * top - p) for core in (0, 1)]
    peers.append(my_e + 1 - 2 * c)

    def dispatch(k):
        plan = []
        if k == 1:
            plan.append((half, lax.rem(g + half, groups) * CHIPS + 2 * (1 - p // 2) + odd, 2))
            pltpu.make_async_copy(sb.at[0], rbuf.at[k, 3], r1.at[k]).start()
            pltpu.make_async_copy(wsend.at[0], wrecv.at[k, 3], rw.at[k]).start()
        for d in (2, 1) if k == 0 else (3,):
            b = 2 * ((d - 1) % 2) + odd
            plan.append((d, lax.rem(g + d, groups) * CHIPS + p // 2, b))
            plan.append((groups - d, lax.rem(g + groups - d, groups) * CHIPS + 2 + p // 2, b))
        for send in (sendw, send1):
            for r, dest_z, b in plan:
                send(r, dest_z, k, b).start()

    def dispatched(k):
        n = 4 if k == 0 else 3
        pltpu.make_async_copy(sb.at[pl.ds(0, n)], sb.at[pl.ds(0, n)], s1.at[k]).wait()
        pltpu.make_async_copy(wsend.at[pl.ds(0, n)], wsend.at[pl.ds(0, n)], sw.at[k]).wait()

    row_of = lax.broadcasted_iota(jnp.int32, (32, 64), 0) // SLOTS
    lane_of = lax.rem(lax.broadcasted_iota(jnp.int32, (32, 64), 1) // 2, 4)
    diagonal = row_of == lane_of
    slot_of = lax.rem(lax.broadcasted_iota(jnp.int32, (32, 128), 0), SLOTS)
    in_slot = lax.broadcasted_iota(jnp.int32, (32, 128), 1) // 16 == slot_of
    wide_row = lax.rem(lax.broadcasted_iota(jnp.int32, (128, 64), 0), 16)
    wide_lane = lax.broadcasted_iota(jnp.int32, (128, 64), 1)
    spread = jnp.where(wide_row == wide_lane // 8 * 2 + lax.rem(wide_lane, 2), 1.0, 0.0).astype(BF16)

    def select(k):
        pltpu.make_async_copy(rbuf.at[k], rbuf.at[k], r1.at[k]).wait()
        pltpu.make_async_copy(wrecv.at[k], wrecv.at[k], rw.at[k]).wait()
        weights = jnp.concatenate([jnp.broadcast_to(wrecv[k, b], (SLOTS, 128)) for b in range(4)], axis=0)
        weights = jnp.where(in_slot, weights, 0.0)
        w_hi = weights.astype(BF16)
        w_lo = (weights - w_hi.astype(F32)).astype(BF16)
        high = jnp.where(diagonal, dot(w_hi, spread), 0.0)
        low = jnp.where(diagonal, dot(w_lo, spread), 0.0)
        wmat[k, 0] = high.astype(BF16)
        wmat[k, 1] = low.astype(BF16)
        sel = jnp.where(high != 0.0, 1.0, 0.0).astype(BF16)
        chosen = dot(sel, rbuf[k].reshape(4 * SLOTS, width), ((0,), (0,)))
        for ee in range(EPG):
            sbuf[k, ee] = chosen[ee * 8:(ee + 1) * 8].astype(BF16)
        for ee in peers:
            pltpu.make_async_remote_copy(
                src_ref=sbuf.at[k, ee], dst_ref=xe.at[k, my_e], send_sem=s2, recv_sem=r2.at[k],
                device_id={"ep": g * EPG + ee}, device_id_type=MESH,
            ).start()
        pltpu.make_async_copy(sbuf.at[k, my_e], xe.at[k, my_e], r2.at[k]).start()

    def expert(k):
        pltpu.make_async_copy(xe.at[k], xe.at[k], r2.at[k]).wait()
        x = xe[k].reshape(64, width)
        a = dot(x, gate[...])
        b = dot(x, up[...])
        h = (a / (1.0 + jnp.exp(-a)) * b).astype(BF16)
        y = dot(h, down[...])
        for i in range(EPG):
            yo[k, i] = y[i * 8:(i + 1) * 8].astype(BF16)
        for ee in peers:
            pltpu.make_async_remote_copy(
                src_ref=yo.at[k, ee], dst_ref=pbuf.at[k, my_e], send_sem=s3, recv_sem=r3.at[k],
                device_id={"ep": g * EPG + ee}, device_id_type=MESH,
            ).start()
        pltpu.make_async_copy(yo.at[k, my_e], pbuf.at[k, my_e], r3.at[k]).start()

    def combine(k):
        pltpu.make_async_copy(pbuf.at[k], pbuf.at[k], r3.at[k]).wait()
        parts = pbuf[k].reshape(64, width)
        y = dot(wmat[k, 0], parts) + dot(wmat[k, 1], parts)
        for b in range(4):
            obuf[k, b] = y[b * 8:(b + 1) * 8].astype(BF16)
        if k == 1:
            pltpu.make_async_copy(obuf.at[k, 3], ret.at[0], r4).start()

    def returns():
        sign = 1 - 2 * (p // 2)
        found = []
        for d in (1, 2, 3):
            for i in range(2):
                src_z = lax.rem(g + groups - sign * d, groups) * CHIPS + 2 * odd + i
                found.append(((d - 1) // 2, 2 * ((d - 1) % 2) + i, src_z, lax.rem(groups + sign * d, groups)))
        found.append((1, 2, lax.rem(g + half, groups) * CHIPS + lax.rem(p + 2, CHIPS), half))
        return found

    def give(name):
        ks, low, high, act = RETURNS[name]
        for k, b, src_z, r in returns():
            if k in ks:
                @pl.when((src_z >= low) & (src_z < high))
                def _():
                    cp = pltpu.make_async_remote_copy(
                        src_ref=obuf.at[k, b], dst_ref=ret.at[r], send_sem=s4.at[k, b], recv_sem=r4,
                        device_id=ep_of(src_z), device_id_type=MESH,
                    )
                    if act:
                        cp.start()
                    else:
                        cp.wait_send()

    for cp in weight_copies:
        cp.wait()
    phases = {"H": hear, "D": dispatch, "W": dispatched, "S": select, "E": expert, "C": combine}
    for step in ORDER:
        if step in RETURNS:
            give(step)
        else:
            phases[step[0]](int(step[1]))

    pltpu.make_async_copy(ret, ret, r4).wait()
    mixed = dot(unplace, ret[...].reshape(groups * SLOTS, width))
    for i in range(tp_count):
        mx[i] = mixed[:, i * piece:(i + 1) * piece].astype(BF16)
    mine = pltpu.make_async_copy(mx.at[t], out.at[pl.ds(t * rows, rows)], in_sem.at[2])
    mine.start()
    if tp_count > 1:
        for dy, dx in PLANE:
            peer = lax.rem(t // CHIPS + dy, CHIPS) * CHIPS + lax.rem(t + dx, CHIPS)
            pltpu.make_async_remote_copy(
                src_ref=mx.at[peer], dst_ref=out.at[pl.ds(t * rows, rows)],
                send_sem=fin_send, recv_sem=fin_recv, device_id={"tp": peer}, device_id_type=MESH,
            ).start()

        others = mx.at[pl.ds(0, tp_count - 1)]
        pltpu.make_async_copy(others, others, fin_recv).wait()
        pltpu.make_async_copy(others, others, fin_send).wait()
        others = xin.at[pl.ds(0, tp_count - 1)]
        pltpu.make_async_copy(others, others, tp_send).wait()
    mine.wait()

    for k in range(NB):
        if "W%d" % k not in ORDER:
            dispatched(k)
    give("W")
    for src, sem in ((sbuf, s2), (yo, s3)):
        every = src.at[:, pl.ds(0, EPG - 1)]
        pltpu.make_async_copy(every, every, sem).wait()


def local(tokens, norm_gain, gate_weight, up_weight, down_weight, expert_ids, route_weight, ep_count, tp_count):
    tok, piece = tokens.shape
    rows = tok // tp_count
    _, width, ff = gate_weight.shape
    groups = ep_count // EPG
    nb = NB
    any_spec = pl.BlockSpec(memory_space=pl.ANY)
    dma = pltpu.SemaphoreType.DMA
    return pl.pallas_call(
        partial(body, ep_count, tp_count),
        out_shape=jax.ShapeDtypeStruct(tokens.shape, BF16),
        in_specs=[any_spec] * 7,
        out_specs=any_spec,
        scratch_shapes=[
            pltpu.VMEM((tok, piece), BF16),
            pltpu.VMEM((tp_count, rows, piece), BF16),
            pltpu.VMEM((1, width), F32),
            pltpu.VMEM((2, tok), jnp.int32),
            pltpu.VMEM((2, tok), F32),
            pltpu.VMEM((width, ff), BF16),
            pltpu.VMEM((width, ff), BF16),
            pltpu.VMEM((ff, width), BF16),
            pltpu.VMEM((rows, width), BF16),
            pltpu.VMEM((groups, SLOTS, width), BF16),
            pltpu.VMEM((nb, 4, SLOTS, width), BF16),
            pltpu.VMEM((nb, EPG, 8, width), BF16),
            pltpu.VMEM((nb, EPG, 8, width), BF16),
            pltpu.VMEM((nb, EPG, 8, width), BF16),
            pltpu.VMEM((nb, EPG, 8, width), BF16),
            pltpu.VMEM((nb, 4, SLOTS, width), BF16),
            pltpu.VMEM((groups, SLOTS, width), BF16),
            pltpu.VMEM((tp_count, rows, piece), BF16),
            pltpu.VMEM((groups, 1, 128), F32),
            pltpu.VMEM((nb, 4, 1, 128), F32),
            pltpu.VMEM((nb, 2, 32, 64), BF16),
            pltpu.SemaphoreType.REGULAR((8,)),
            dma((nb,)), dma((nb,)),
            dma((3,)), dma((4,)), dma, dma,
            dma((nb,)), dma((nb,)), dma, dma((nb,)), dma, dma((nb,)), dma((nb, 4)), dma, dma, dma,
        ],
        compiler_params=pltpu.CompilerParams(
            collective_id=0, has_side_effects=True, vmem_limit_bytes=67043328
        ),
        name="moe",
    )(tokens, norm_gain.reshape(1, width), gate_weight, up_weight, down_weight, expert_ids.T, route_weight.T)


def solution(mesh):
    in_specs = (
        P("ep", "tp"),
        P(),
        P("ep", None, None),
        P("ep", None, None),
        P("ep", None, None),
        P("ep", None),
        P("ep", None),
    )
    fn = partial(local, ep_count=mesh.shape["ep"], tp_count=mesh.shape["tp"])
    return jax.shard_map(fn, mesh=mesh, in_specs=in_specs, out_specs=P("ep", "tp"), check_vma=False)
```
